32 devices in a mesh: grp: 2 (over y), tp: 4 (over z), dp: 4 (over x, core).
Axes of the slice: x: 2, y: 2, z: 4, core: 2. Of those that a mesh axis runs over, the one named last changes fastest.
Arguments:
- tokens: bfloat16 [64, 4096], P(('grp', 'tp'), 'dp'), parts along dimension 0, may hold values from -50 to 50
- norm_gain: float32 [2, 4096], P(None, 'dp'), may hold values from 0.1 to 1.9
- query_weight: bfloat16 [2, 4096, 4096], P(None, 'dp', 'tp'), may hold values from -0.09375 to 0.09375
- key_weight: bfloat16 [2, 4096, 4096], P(None, 'dp', 'tp'), may hold values from -0.09375 to 0.09375
- value_weight: bfloat16 [2, 4096, 4096], P(None, 'dp', 'tp'), may hold values from -0.09375 to 0.09375
- outgate_weight: bfloat16 [2, 4096, 4096], P(None, 'dp', 'tp'), may hold values from -0.09375 to 0.09375
- input_gate_weight: bfloat16 [2, 4096, 64], P(None, 'dp', 'tp'), may hold values from -0.09375 to 0.09375
- forget_gate_weight: bfloat16 [2, 4096, 64], P(None, 'dp', 'tp'), may hold values from -0.09375 to 0.09375
- forget_bias: float32 [2, 64], P(None, 'tp'), may hold values from -2 to 5
- out_weight: bfloat16 [2, 4096, 4096], P(None, 'tp', 'dp'), may hold values from -0.09375 to 0.09375
- memory_state: float32 [2, 64, 64, 4096], P(None, ('grp', 'dp'), 'tp'), parts along dimension 1, may hold values from -0.9 to 0.9
- normalizer_state: float32 [2, 64, 4096], P(None, ('grp', 'dp'), 'tp'), parts along dimension 1, may hold values from -0.9 to 0.9
- maximum_state: float32 [2, 64, 64], P(None, ('grp', 'dp'), 'tp'), parts along dimension 1, may hold values from -1 to 1
Outputs:
- next_tokens: bfloat16 [64, 4096], P(('grp', 'tp'), 'dp'), parts along dimension 0
- next_memory: float32 [2, 64, 64, 4096], P(None, ('grp', 'dp'), 'tp'), parts along dimension 1
- next_normalizer: float32 [2, 64, 4096], P(None, ('grp', 'dp'), 'tp'), parts along dimension 1
- next_maximum: float32 [2, 64, 64], P(None, ('grp', 'dp'), 'tp'), parts along dimension 1
The draws below stay inside these ranges and needn't reach their ends.
There are 2 independent parts, one for each index of `grp`. The reference program is written for one: setup_inputs(seed, part) draws one part's arguments, and reference() takes and returns one part's arrays. A program takes and returns all parts, laid end to end along the dimension named above; an argument that names none is the same for every part. Nothing has to cross between parts.
All inputs are finite; a program needn't handle non-finite values.
Results may differ from the reference program's by a relative error of at most 0.0074.
Values may be sent and summed in bfloat16 or wider, within the bound.
A program may use at most 128 MiB of HBM per device.

```python
import math
import jax
import jax.numpy as jnp
from jax import lax

D = 4096
HEADS = 64
HEAD = 64
LAYERS = 2
BATCH = 32


def draw_tokens(key, part):
    key_entries = jax.random.fold_in(key, 11)
    key_rows = jax.random.fold_in(key, 12)
    columns = jnp.arange(D, dtype=jnp.float32) / (D - 1) - 0.5
    row_scale = jnp.exp(jax.random.uniform(key_rows, (BATCH, 1), jnp.float32, -1.15, 1.15))
    entries = jnp.clip(jax.random.normal(key_entries, (BATCH, D), jnp.float32), -5.0, 5.0)
    column_ramp = jnp.exp(math.log(10.0) * columns)
    return (entries * row_scale * column_ramp[None, :]).astype(jnp.bfloat16)


def levels(rng, extent, pieces, least, largest):
    def one(position, shards_of):
        steps = jax.random.uniform(jax.random.fold_in(jax.random.fold_in(rng, 6), position), (shards_of,), jnp.float32, least / len(pieces), largest / len(pieces))
        return jnp.repeat(jnp.exp(steps), extent[position] // shards_of).reshape((-1,) + (1,) * (len(extent) - position - 1))

    level = one(*pieces[0])
    for cut in pieces[1:]:
        level = level * one(*cut)
    return level


def scatter_about(key, dims, width, bound, cuts=(), kind=jnp.bfloat16):
    drawn = width * jax.random.normal(key, dims, jnp.float32)
    if cuts:
        drawn = drawn * levels(key, dims, cuts, -0.22, 0.18)
    return jnp.clip(drawn, -bound, bound).astype(kind)


def setup_inputs(seed: int = 0, part: int = 0) -> dict:
    streams_of = jax.random.split(jax.random.key(seed), 14)
    own_keys = jax.random.split(jax.random.fold_in(streams_of[13], part), 14)
    return {
        "tokens": draw_tokens(jax.random.fold_in(jax.random.fold_in(streams_of[13], part), 71), part),
        "norm_gain": jnp.clip(1.0 + 0.18 * jax.random.normal(streams_of[1], (LAYERS, D), jnp.float32), 0.1, 1.9),
        "query_weight": scatter_about(streams_of[2], (LAYERS, D, HEADS * HEAD), D ** -0.5, 0.09375, ((1, 4), (2, 4))),
        "key_weight": scatter_about(streams_of[3], (LAYERS, D, HEADS * HEAD), D ** -0.5, 0.09375, ((1, 4), (2, 4))),
        "value_weight": scatter_about(streams_of[4], (LAYERS, D, HEADS * HEAD), D ** -0.5, 0.09375, ((1, 4), (2, 4))),
        "outgate_weight": scatter_about(streams_of[5], (LAYERS, D, HEADS * HEAD), D ** -0.5, 0.09375, ((1, 4), (2, 4))),
        "input_gate_weight": scatter_about(streams_of[6], (LAYERS, D, HEADS), D ** -0.5, 0.09375, ((1, 4), (2, 4))),
        "forget_gate_weight": scatter_about(streams_of[7], (LAYERS, D, HEADS), D ** -0.5, 0.09375, ((1, 4), (2, 4))),
        "forget_bias": jnp.clip(-2.0 + 7.0 * jax.random.uniform(streams_of[8], (LAYERS, HEADS), jnp.float32) ** levels(streams_of[8], (LAYERS, HEADS), ((1, 4),), -0.2, 0.2), -2.0, 5.0),
        "out_weight": scatter_about(streams_of[9], (LAYERS, HEADS * HEAD, D), (HEADS * HEAD) ** -0.5, 0.09375, ((1, 4), (2, 4))),
        "memory_state": scatter_about(own_keys[10], (LAYERS, BATCH, HEADS, HEAD * HEAD), 0.15, 0.9, ((1, 4), (2, 4)), jnp.float32),
        "normalizer_state": scatter_about(own_keys[11], (LAYERS, BATCH, HEADS * HEAD), 0.15, 0.9, ((1, 4), (2, 4)), jnp.float32),
        "maximum_state": jnp.clip(jax.random.uniform(own_keys[12], (LAYERS, BATCH, HEADS), jnp.float32, -1.0, 1.0) * levels(own_keys[12], (LAYERS, BATCH, HEADS), ((1, 4), (2, 4)), -0.4, 0.0), -1.0, 1.0),
    }


EPS = 1e-06

def reference(tokens, norm_gain, query_weight, key_weight, value_weight, outgate_weight, input_gate_weight, forget_gate_weight, forget_bias, out_weight, memory_state, normalizer_state, maximum_state):
    current = tokens
    memories = []
    normalizers = []
    maxima = []
    batch_rows = tokens.shape[0]
    shape = (batch_rows, HEADS, HEAD)
    for layer_idx in range(LAYERS):
        x_float = current.astype(jnp.float32)
        squares = lax.optimization_barrier(jnp.sum(x_float * x_float, axis=1))
        inv_rms = lax.rsqrt(squares / D + EPS)[:, None]
        scaled = (x_float * norm_gain[layer_idx][None, :]).astype(jnp.bfloat16)

        def project(weight):
            return inv_rms * jnp.dot(scaled, weight, preferred_element_type=jnp.float32)

        def rounded(weight):
            stored = lax.optimization_barrier(project(weight).astype(jnp.bfloat16))
            return stored.astype(jnp.float32).reshape(shape)
        query_vec = rounded(query_weight[layer_idx])
        key_vec = rounded(key_weight[layer_idx]) * HEAD ** (-0.5)
        value_vec = rounded(value_weight[layer_idx])
        gate_vec = rounded(outgate_weight[layer_idx])
        input_pre = project(input_gate_weight[layer_idx])
        forget_pre = project(forget_gate_weight[layer_idx]) + forget_bias[layer_idx][None, :]
        log_forget = jax.nn.log_sigmoid(forget_pre)
        old_max = maximum_state[layer_idx]
        new_max = jnp.maximum(log_forget + old_max, input_pre)
        keep_rate = jnp.exp(log_forget + old_max - new_max)
        admit_rate = jnp.exp(input_pre - new_max)
        memory = memory_state[layer_idx].reshape(batch_rows, HEADS, HEAD, HEAD)
        memory = keep_rate[:, :, None, None] * memory + admit_rate[:, :, None, None] * key_vec[:, :, :, None] * value_vec[:, :, None, :]
        normalizer = keep_rate[:, :, None] * normalizer_state[layer_idx].reshape(shape) + admit_rate[:, :, None] * key_vec
        numerator = jnp.einsum('bhd,bhde->bhe', query_vec, memory, precision=lax.Precision.HIGHEST)
        denominator = lax.optimization_barrier(jnp.sum(query_vec * normalizer, axis=2))
        readout = numerator / jnp.maximum(jnp.abs(denominator), jnp.exp(-new_max))[:, :, None]
        mixed = (readout * jax.nn.sigmoid(gate_vec)).astype(jnp.bfloat16).reshape(batch_rows, HEADS * HEAD)
        summed = jnp.dot(mixed, out_weight[layer_idx], preferred_element_type=jnp.float32)
        current = (x_float + summed).astype(jnp.bfloat16)
        memories.append(memory.reshape(batch_rows, HEADS, HEAD * HEAD))
        normalizers.append(normalizer.reshape(batch_rows, HEADS * HEAD))
        maxima.append(new_max)
    return (current, jnp.stack(memories), jnp.stack(normalizers), jnp.stack(maxima))
```

```python
import functools

import jax
import jax.numpy as jnp
from jax import lax
from jax.experimental import pallas as pl
from jax.experimental.pallas import tpu as pltpu
from jax.sharding import PartitionSpec as P

EPS = 1e-06
F32 = jnp.float32
BF16 = jnp.bfloat16
MESH = pl.DeviceIdType.MESH
LANES = 128


def dot(a, b):
    return jnp.dot(a, b, preferred_element_type=F32)


def dot_t(a, b):
    return lax.dot_general(a, b, (((1,), (1,)), ((), ())), preferred_element_type=F32)


def iota(shape, dim):
    return lax.broadcasted_iota(jnp.int32, shape, dim)


def kernel(
    n_tp,
    n_dp,
    tokens,
    gain_in,
    wq,
    wk,
    wv,
    wg,
    wi_in,
    wf_in,
    bias_in,
    wo,
    mem_in,
    norm_in,
    max_in,
    tok_out,
    m,
    norm_out,
    max_out,
    x_all,
    gain,
    w,
    wi,
    wf,
    bias,
    norm,
    maxs,
    spread,
    fold,
    unfold,
    mask,
    p_own,
    p_send,
    p_recv,
    g_send,
    g_recv,
    mix_all,
    o_own,
    o_send,
    o_recv,
    load_sem,
    w_sem,
    m_sem,
    x_ss,
    x_rs,
    p_ss,
    p_rs,
    g_ss,
    g_rs,
    mix_ss,
    mix_rs,
    o_ss,
    o_rs,
):
    t = lax.axis_index("tp")
    d = lax.axis_index("dp")
    layers = wq.shape[0]
    rows_x, d_local = tokens.shape
    width = wq.shape[2]
    seqs, heads, square = mem_in.shape[1:]
    hd = width // heads
    hd_bits = hd.bit_length() - 1
    hp = mask.shape[0] // seqs
    rows = seqs * hp
    batch = n_tp * rows_x
    depth = d_local * n_dp
    pair = fold.shape[1]

    loads = [
        pltpu.make_async_copy(src, dst, load_sem.at[i])
        for i, (src, dst) in enumerate(
            [
                (tokens, x_all.at[0, t]),
                (gain_in, gain),
                (wi_in, wi),
                (wf_in, wf),
                (bias_in, bias),
                (max_in, maxs),
                (norm_in, norm),
            ]
        )
    ]
    for c in loads:
        c.start()
    order = (wq, wk, wv, wg, wo)
    w_loads = [
        [pltpu.make_async_copy(order[c].at[l], w.at[l, c], w_sem.at[l, c]) for c in range(5)]
        for l in range(layers)
    ]
    m_loads = [pltpu.make_async_copy(mem_in.at[l], m.at[l], m_sem.at[l]) for l in range(layers)]

    def start_loads(l, first, last):
        for c in range(first, last):
            w_loads[l][c].start()

    start_loads(0, 0, 4)
    m_loads[0].start()
    barrier = pltpu.get_barrier_semaphore()
    for o in range(1, n_tp):
        pl.semaphore_signal(
            barrier, inc=1, device_id={"tp": lax.rem(t + o, n_tp)}, device_id_type=MESH
        )
    for o in range(1, n_dp):
        pl.semaphore_signal(
            barrier, inc=1, device_id={"dp": lax.rem(d + o, n_dp)}, device_id_type=MESH
        )
    pl.semaphore_wait(barrier, n_tp + n_dp - 2)
    loads[0].wait()

    sends = []

    def send(src, dst, ss, rs, axis, peer):
        copy = pltpu.make_async_remote_copy(
            src_ref=src,
            dst_ref=dst,
            send_sem=ss,
            recv_sem=rs,
            device_id={axis: peer},
            device_id_type=MESH,
        )
        copy.start()
        sends.append(copy)
        return copy

    def send_x(l):
        return [
            send(
                x_all.at[l, t],
                x_all.at[l, t],
                x_ss.at[l, o - 1],
                x_rs.at[l, o - 1],
                "tp",
                lax.rem(t + o, n_tp),
            )
            for o in range(1, n_tp)
        ]

    x_copies = send_x(0)
    start_loads(0, 4, 5)

    spread[...] = jnp.where(
        lax.shift_right_logical(iota(spread.shape, 1), hd_bits) == iota(spread.shape, 0), 1.0, 0.0
    ).astype(BF16)
    fold[...] = jnp.where(
        (iota(fold.shape, 0) & (hd - 1)) == (iota(fold.shape, 1) & (hd - 1)), 1.0, 0.0
    ).astype(BF16)
    unfold[...] = jnp.where(
        iota(unfold.shape, 0) == (iota(unfold.shape, 1) & (hd - 1)), 1.0, 0.0
    ).astype(BF16)
    mask[...] = jnp.where(
        (iota(mask.shape, 0) & (hp - 1)) == lax.shift_right_logical(iota(mask.shape, 1), hd_bits),
        1.0,
        0.0,
    )

    def over_heads(z):
        return jnp.broadcast_to(z[:, None, :], (seqs, hp, z.shape[1])).reshape(rows, z.shape[1])

    def column(z):
        own = (iota((rows, heads), 0) & (hp - 1)) == iota((rows, heads), 1)
        return jnp.sum(jnp.where(own, over_heads(z), 0.0), axis=1, keepdims=True)

    def to_rows(z):
        return dot((over_heads(z) * mask[...]).astype(BF16), fold[...])

    def from_rows(z):
        return jnp.sum(z.reshape(seqs, hp, width), axis=1)

    def three(z):
        return z.reshape(seqs, hp, z.shape[1])[:, 0:heads]

    for c in loads[1:]:
        c.wait()

    for l in range(layers):
        for c in x_copies:
            c.wait_recv()
        x = x_all[l].astype(F32).reshape(batch, d_local)
        squares = jnp.sum(x * x, axis=1, keepdims=True)
        scaled = (x * gain[l : l + 1, :]).astype(BF16)
        g_terms = jnp.concatenate(
            [
                dot_t(scaled, wi[l]),
                dot_t(scaled, wf[l]),
                jnp.broadcast_to(squares, (batch, LANES - 2 * heads)),
            ],
            axis=1,
        )
        g_send[l] = g_terms.reshape(n_dp, seqs, LANES)
        g_copies = [
            send(
                g_send.at[l, lax.rem(d + o, n_dp)],
                g_recv.at[l, o - 1],
                g_ss.at[l, o - 1],
                g_rs.at[l, o - 1],
                "dp",
                lax.rem(d + o, n_dp),
            )
            for o in range(1, n_dp)
        ]
        p_copies = []
        for c in range(4):
            w_loads[l][c].wait()
            product = dot(scaled, w[l, c]).reshape(n_dp, seqs, width)
            p_own[c] = product
            p_send[l, c] = product.astype(BF16)
            p_copies.append(
                [
                    send(
                        p_send.at[l, c, lax.rem(d + o, n_dp)],
                        p_recv.at[l, c, o - 1],
                        p_ss.at[l, c, o - 1],
                        p_rs.at[l, c, o - 1],
                        "dp",
                        lax.rem(d + o, n_dp),
                    )
                    for o in range(1, n_dp)
                ]
            )

        if l + 1 < layers:
            start_loads(l + 1, 0, 4)
            m_loads[l + 1].start()
            start_loads(l + 1, 4, 5)

        for c in g_copies:
            c.wait_recv()
        g_sum = g_send[l, d]
        for o in range(1, n_dp):
            g_sum = g_sum + g_recv[l, o - 1]
        inv_rms = lax.rsqrt(g_sum[:, 2 * heads : 2 * heads + 1] / depth + EPS)
        input_pre = inv_rms * g_sum[:, 0:heads]
        forget_pre = inv_rms * g_sum[:, heads : 2 * heads] + bias[l : l + 1, :]
        log_forget = jnp.minimum(forget_pre, 0.0) - jnp.log1p(jnp.exp(-jnp.abs(forget_pre)))
        old_max = maxs[l]
        new_max = jnp.maximum(log_forget + old_max, input_pre)
        max_out[l] = new_max
        keep = column(jnp.exp(log_forget + old_max - new_max))
        admit = column(jnp.exp(input_pre - new_max))
        floor = column(jnp.exp(-new_max))
        if hp != heads:
            floor = jnp.where((iota((rows, 1), 0) & (hp - 1)) < heads, floor, 1.0)
        keep_wide = from_rows(keep * mask[...])
        admit_wide = from_rows(admit * mask[...])

        def stored(c):
            for copy in p_copies[c]:
                copy.wait_recv()
            total = p_own[c, d]
            for o in range(1, n_dp):
                total = total + p_recv[l, c, o - 1].astype(F32)
            return (inv_rms * total).astype(BF16).astype(F32)

        query = stored(0)
        query_rows = to_rows(query).astype(BF16)
        m_loads[l].wait()
        step = 2 * pair

        def read(j, acc):
            qx = dot(query_rows, spread[:, pl.ds(pl.multiple_of(j * step, step), step)])
            for i in range(2):
                at = pl.ds(pl.multiple_of(j * step + i * pair, pair), pair)
                acc = acc + three(qx[:, i * pair : (i + 1) * pair]) * m[l, :, :, at]
            return acc

        acc = lax.fori_loop(0, square // step, read, jnp.zeros((seqs, heads, pair), F32), unroll=True)
        key = stored(1) * hd ** (-0.5)
        new_norm = keep_wide * norm[l] + admit_wide * key
        norm_out[l] = new_norm
        key_rows = to_rows(key).astype(BF16)
        inner = jnp.sum(over_heads(query * new_norm) * mask[...], axis=1, keepdims=True)
        match = jnp.sum(over_heads(query * key) * mask[...], axis=1, keepdims=True)
        admitted = admit * to_rows(stored(2))
        gate = jax.nn.sigmoid(to_rows(stored(3)))
        if hp != heads:
            acc = jnp.concatenate([acc, jnp.zeros((seqs, hp - heads, pair), F32)], axis=1)
        acc = acc.reshape(rows, pair)
        acc = acc + pltpu.roll(acc, hd, 1)
        readout = (keep * acc + match * admitted) / jnp.maximum(jnp.abs(inner), floor)
        mixed = (readout * gate).astype(BF16)
        mix_all[l, d] = from_rows(dot(mixed, unfold[...]) * mask[...]).astype(BF16)
        mix_copies = [
            send(
                mix_all.at[l, d],
                mix_all.at[l, d],
                mix_ss.at[l, o - 1],
                mix_rs.at[l, o - 1],
                "dp",
                lax.rem(d + o, n_dp),
            )
            for o in range(1, n_dp)
        ]
        keep3 = three(jnp.broadcast_to(keep, (rows, pair)))
        admitted3 = three(admitted)

        @pl.loop(0, square // step, unroll=True)
        def update(j):
            kx = dot(key_rows, spread[:, pl.ds(pl.multiple_of(j * step, step), step)])
            for i in range(2):
                at = pl.ds(pl.multiple_of(j * step + i * pair, pair), pair)
                part = three(kx[:, i * pair : (i + 1) * pair])
                m[l, :, :, at] = keep3 * m[l, :, :, at] + part * admitted3

        w_loads[l][4].wait()
        for c in mix_copies:
            c.wait_recv()
        mixed_all = mix_all[l].astype(F32).reshape(batch, width).astype(BF16)
        partial_out = dot(mixed_all, w[l, 4]).reshape(n_tp, rows_x, d_local)
        o_own[...] = partial_out
        o_send[l] = partial_out.astype(BF16)
        o_copies = [
            send(
                o_send.at[l, lax.rem(t + o, n_tp)],
                o_recv.at[l, o - 1],
                o_ss.at[l, o - 1],
                o_rs.at[l, o - 1],
                "tp",
                lax.rem(t + o, n_tp),
            )
            for o in range(1, n_tp)
        ]
        total = o_own[t]
        for o in range(1, n_tp):
            o_copies[o - 1].wait_recv()
            total = total + o_recv[l, o - 1].astype(F32)
        result = (x_all[l, t].astype(F32) + total).astype(BF16)
        if l + 1 < layers:
            x_all[l + 1, t] = result
            x_copies = send_x(l + 1)
        else:
            tok_out[...] = result

    for c in sends:
        c.wait_send()


def store(*refs):
    n = len(refs) // 2
    copies = [pltpu.make_async_copy(refs[i], refs[n + i], refs[-1].at[i]) for i in range(n)]
    for c in copies:
        c.start()
    for c in copies:
        c.wait()


def solution(mesh):
    n_tp, n_dp = mesh.shape["tp"], mesh.shape["dp"]

    def per_device(
        tokens,
        norm_gain,
        query_weight,
        key_weight,
        value_weight,
        outgate_weight,
        input_gate_weight,
        forget_gate_weight,
        forget_bias,
        out_weight,
        memory_state,
        normalizer_state,
        maximum_state,
    ):
        rows_x, d_local = tokens.shape
        layers, _, width = query_weight.shape
        _, seqs, heads, square = memory_state.shape
        hd = width // heads
        hp = -(-heads // 8) * 8
        sem = pltpu.SemaphoreType.DMA
        vmem = pltpu.VMEM
        anywhere = pl.BlockSpec(memory_space=pl.ANY)
        in_vmem = pl.BlockSpec(memory_space=pltpu.VMEM)
        results = [
            (tokens.shape, BF16),
            (memory_state.shape, F32),
            (normalizer_state.shape, F32),
            (maximum_state.shape, F32),
        ]
        room = memory_state.size * 4 + normalizer_state.size * 4
        limit = (60 << 20) + (3 << 20) - max(room, 3 << 20) - (256 << 10)
        held = pl.pallas_call(
            functools.partial(kernel, n_tp, n_dp),
            out_shape=tuple(vmem(*r) for r in results),
            in_specs=[anywhere] * 13,
            out_specs=(in_vmem,) * 4,
            scratch_shapes=[
                vmem((layers, n_tp, rows_x, d_local), BF16),
                vmem(norm_gain.shape, F32),
                vmem((layers, 5, d_local, width), BF16),
                vmem((layers, heads, d_local), BF16),
                vmem((layers, heads, d_local), BF16),
                vmem(forget_bias.shape, F32),
                vmem(normalizer_state.shape, F32),
                vmem(maximum_state.shape, F32),
                vmem((2 * hd, square), BF16),
                vmem((width, 2 * hd), BF16),
                vmem((2 * hd, width), BF16),
                vmem((seqs * hp, width), F32),
                vmem((4, n_dp, seqs, width), F32),
                vmem((layers, 4, n_dp, seqs, width), BF16),
                vmem((layers, 4, n_dp - 1, seqs, width), BF16),
                vmem((layers, n_dp, seqs, LANES), F32),
                vmem((layers, n_dp - 1, seqs, LANES), F32),
                vmem((layers, n_dp, seqs, width), BF16),
                vmem((n_tp, rows_x, d_local), F32),
                vmem((layers, n_tp, rows_x, d_local), BF16),
                vmem((layers, n_tp - 1, rows_x, d_local), BF16),
                sem((7,)),
                sem((layers, 5)),
                sem((layers,)),
                sem((layers, n_tp - 1)),
                sem((layers, n_tp - 1)),
                sem((layers, 4, n_dp - 1)),
                sem((layers, 4, n_dp - 1)),
                sem((layers, n_dp - 1)),
                sem((layers, n_dp - 1)),
                sem((layers, n_dp - 1)),
                sem((layers, n_dp - 1)),
                sem((layers, n_tp - 1)),
                sem((layers, n_tp - 1)),
            ],
            compiler_params=pltpu.CompilerParams(
                collective_id=0, has_side_effects=True, vmem_limit_bytes=limit
            ),
        )(
            tokens,
            norm_gain,
            query_weight,
            key_weight,
            value_weight,
            outgate_weight,
            jnp.swapaxes(input_gate_weight, 1, 2),
            jnp.swapaxes(forget_gate_weight, 1, 2),
            forget_bias,
            out_weight,
            memory_state,
            normalizer_state,
            maximum_state,
        )
        return pl.pallas_call(
            store,
            out_shape=tuple(jax.ShapeDtypeStruct(*r) for r in results),
            in_specs=[in_vmem] * 4,
            out_specs=(anywhere,) * 4,
            scratch_shapes=[sem((4,))],
            compiler_params=pltpu.CompilerParams(vmem_limit_bytes=1024 * 1024),
        )(*held)

    in_specs = (
        P(("grp", "tp"), "dp"),
        P(None, "dp"),
        P(None, "dp", "tp"),
        P(None, "dp", "tp"),
        P(None, "dp", "tp"),
        P(None, "dp", "tp"),
        P(None, "dp", "tp"),
        P(None, "dp", "tp"),
        P(None, "tp"),
        P(None, "tp", "dp"),
        P(None, ("grp", "dp"), "tp", None),
        P(None, ("grp", "dp"), "tp"),
        P(None, ("grp", "dp"), "tp"),
    )
    out_specs = (
        P(("grp", "tp"), "dp"),
        P(None, ("grp", "dp"), "tp", None),
        P(None, ("grp", "dp"), "tp"),
        P(None, ("grp", "dp"), "tp"),
    )
    return jax.shard_map(
        per_device, mesh=mesh, in_specs=in_specs, out_specs=out_specs, check_vma=False
    )
```

```python
import functools

import jax
import jax.numpy as jnp
from jax import lax
from jax.experimental import pallas as pl
from jax.experimental.pallas import tpu as pltpu
from jax.sharding import PartitionSpec as P

EPS = 1e-06
F32 = jnp.float32
BF16 = jnp.bfloat16
MESH = pl.DeviceIdType.MESH
LANES = 128


def dot(a, b):
    return jnp.dot(a, b, preferred_element_type=F32)


def dot_t(a, b):
    return lax.dot_general(a, b, (((1,), (1,)), ((), ())), preferred_element_type=F32)


def iota(shape, dim):
    return lax.broadcasted_iota(jnp.int32, shape, dim)


def kernel(
    n_tp,
    n_dp,
    tokens,
    gain_in,
    wq,
    wk,
    wv,
    wg,
    wi_in,
    wf_in,
    bias_in,
    wo,
    mem_in,
    norm_in,
    max_in,
    tok_out,
    m,
    norm_out,
    max_out,
    x_all,
    xs,
    gain,
    w,
    wi,
    wf,
    wif,
    bias,
    norm,
    maxs,
    spread,
    fold,
    unfold,
    mask,
    p_own,
    p_send,
    p_near,
    p_recv,
    p_pair,
    p_both,
    p_sum,
    p_far,
    g_send,
    g_recv,
    mix_all,
    o_own,
    o_send,
    o_recv,
    r_own,
    r_send,
    r_recv,
    load_sem,
    w_sem,
    m_sem,
    x_ss,
    x_rs,
    p_ss,
    p_rs,
    g_ss,
    g_rs,
    mix_ss,
    mix_rs,
    o_ss,
    o_rs,
    first_ss,
    first_rs,
    r_ss,
    r_rs,
    pair_ss,
    pair_rs,
    far_ss,
    far_rs,
):
    t = lax.axis_index("tp")
    d = lax.axis_index("dp")
    layers = wq.shape[0]
    rows_x, d_local = tokens.shape
    width = wq.shape[2]
    seqs, heads, square = mem_in.shape[1:]
    hd = width // heads
    hd_bits = hd.bit_length() - 1
    hp = mask.shape[0] // seqs
    rows = seqs * hp
    batch = n_tp * rows_x
    depth = d_local * n_dp
    pair = fold.shape[1]
    pieces = o_own.shape[0]
    cut = d_local // pieces
    spans = [slice(j * cut, (j + 1) * cut) for j in range(pieces)]

    loads = [
        pltpu.make_async_copy(src, dst, load_sem.at[i])
        for i, (src, dst) in enumerate(
            [
                (tokens, x_all.at[t]),
                (gain_in, gain),
                (wi_in, wi),
                (wf_in, wf),
                (bias_in, bias),
                (max_in, maxs),
                (norm_in, norm),
            ]
        )
    ]
    for c in loads:
        c.start()
    order = (wq, wk, wv, wg, wo)
    w_loads = [
        [pltpu.make_async_copy(order[c].at[l], w.at[l, c], w_sem.at[l, c]) for c in range(5)]
        for l in range(layers)
    ]
    m_loads = [pltpu.make_async_copy(mem_in.at[l], m.at[l], m_sem.at[l]) for l in range(layers)]

    def start_loads(l, first, last):
        for c in range(first, last):
            w_loads[l][c].start()

    start_loads(0, 0, 4)
    m_loads[0].start()
    barrier = pltpu.get_barrier_semaphore()
    for o in range(1, n_tp):
        pl.semaphore_signal(
            barrier, inc=1, device_id={"tp": lax.rem(t + o, n_tp)}, device_id_type=MESH
        )
    for o in range(1, n_dp):
        pl.semaphore_signal(
            barrier, inc=1, device_id={"dp": lax.rem(d + o, n_dp)}, device_id_type=MESH
        )
    pl.semaphore_wait(barrier, n_tp + n_dp - 2)
    loads[0].wait()

    def sibling(e):
        return e + 1 - 2 * lax.rem(e, 2)

    far = []
    for j in range(n_dp // 2):
        e = lax.rem(d + 2 * j, n_dp)
        if j:
            far.append(e)
            far.append(sibling(e))
    near = sibling(d)
    peers = far + [near]
    pairs = [2 * lax.rem(d // 2 + j, n_dp // 2) for j in range(1, n_dp // 2)]
    mine = [lax.rem(d + 2 * j, n_dp) for j in range(n_dp // 2)]
    theirs = [lax.rem(near + 2 * j, n_dp) for j in range(n_dp // 2)]
    tp_peers = [lax.rem(t + o, n_tp) for o in range(1, n_tp)]
    tp_order = tp_peers
    if n_tp % 2 == 0:
        half = n_tp // 2
        upper = t // half
        tp_order = [(1 - upper) * (n_tp - 1) + (2 * upper - 1) * j for j in range(half)]
        tp_order += [upper * half + lax.rem(t + o, half) for o in range(1, half)]

    sends = []

    def send(src, dst, ss, rs, axis, peer):
        copy = pltpu.make_async_remote_copy(
            src_ref=src,
            dst_ref=dst,
            send_sem=ss,
            recv_sem=rs,
            device_id={axis: peer},
            device_id_type=MESH,
        )
        copy.start()
        sends.append(copy)
        return copy

    def arrived(dst, ss, rs, axis, peer):
        pltpu.make_async_remote_copy(
            src_ref=dst,
            dst_ref=dst,
            send_sem=ss,
            recv_sem=rs,
            device_id={axis: peer},
            device_id_type=MESH,
        ).wait_recv()

    for o, peer in enumerate(tp_order):
        send(x_all.at[t], x_all.at[t], x_ss.at[o], x_rs.at[t], "tp", peer)
    start_loads(0, 4, 5)

    spread[...] = jnp.where(
        lax.shift_right_logical(iota(spread.shape, 1), hd_bits) == iota(spread.shape, 0), 1.0, 0.0
    ).astype(BF16)
    fold[...] = jnp.where(
        (iota(fold.shape, 0) & (hd - 1)) == (iota(fold.shape, 1) & (hd - 1)), 1.0, 0.0
    ).astype(BF16)
    unfold[...] = jnp.where(
        (iota(unfold.shape, 0) & (hd - 1)) == (iota(unfold.shape, 1) & (hd - 1)), 1.0, 0.0
    ).astype(BF16)
    mask[...] = jnp.where(
        (iota(mask.shape, 0) & (hp - 1)) == lax.shift_right_logical(iota(mask.shape, 1), hd_bits),
        1.0,
        0.0,
    )

    def over_heads(z):
        return jnp.broadcast_to(z[:, None, :], (seqs, hp, z.shape[1])).reshape(rows, z.shape[1])

    def column(z):
        own = (iota((rows, heads), 0) & (hp - 1)) == iota((rows, heads), 1)
        return jnp.sum(jnp.where(own, over_heads(z), 0.0), axis=1, keepdims=True)

    def to_rows(z):
        return dot((over_heads(z) * mask[...]).astype(BF16), fold[...])

    def from_rows(z):
        return jnp.sum(z.reshape(seqs, hp, width), axis=1)

    def three(z):
        return z.reshape(seqs, hp, z.shape[1])[:, 0:heads]

    def rounded(z):
        return z.astype(BF16).astype(F32)

    for c in loads[1:]:
        c.wait()
    for l in range(layers):
        gate_rows = jnp.concatenate(
            [
                wi[l].astype(F32),
                wf[l].astype(F32),
                jnp.zeros((LANES - 2 * heads, d_local), F32),
            ],
            axis=0,
        )
        wif[l] = gate_rows.T.astype(BF16)

    o_copies = []
    for l in range(layers):
        squares = jnp.zeros((batch, 1), F32)
        gates = jnp.zeros((batch, LANES), F32)
        p_copies = []

        def send_products(c, product):
            own = product.reshape(n_dp, seqs, width)
            p_own[l, c] = own
            if c < 2:
                p_send[l, c] = own.astype(BF16)

        def start_products(c):
            n = len(far)
            return [
                send(
                    p_send.at[l, c, peer],
                    p_recv.at[l, c, i],
                    p_ss.at[l, c, i],
                    p_rs.at[l, c, i],
                    "dp",
                    peer,
                )
                for i, peer in enumerate(far)
            ] + [
                send(
                    p_own.at[l, c, sibling(d)],
                    p_near.at[l, c],
                    p_ss.at[l, c, n],
                    p_rs.at[l, c, n],
                    "dp",
                    sibling(d),
                )
            ]

        def start_pairs(c):
            return [
                send(
                    p_own.at[l, c, e],
                    p_pair.at[l, c - 2, j],
                    pair_ss.at[l, c - 2, j],
                    pair_rs.at[l, c - 2, j],
                    "dp",
                    near,
                )
                for j, e in enumerate(theirs)
            ]

        def pass_pairs(c):
            for copy in p_copies[c]:
                copy.wait_recv()
            p_both[c - 2] = p_own[l, c, d] + p_pair[l, c - 2, 0]
            copies = []
            for j in range(1, n_dp // 2):
                p_sum[l, c - 2, j - 1] = (p_own[l, c, mine[j]] + p_pair[l, c - 2, j]).astype(BF16)
                copies.append(
                    send(
                        p_sum.at[l, c - 2, j - 1],
                        p_far.at[l, c - 2, j - 1],
                        far_ss.at[l, c - 2, j - 1],
                        far_rs.at[l, c - 2, j - 1],
                        "dp",
                        mine[j],
                    )
                )
            return copies

        steps = spans if l else [slice(0, d_local)]
        for j, span in enumerate(steps):
            if l == 0:
                for peer in tp_peers:
                    arrived(x_all.at[peer], x_ss.at[0], x_rs.at[peer], "tp", peer)
                x = x_all[...].astype(F32).reshape(batch, d_local)
            else:
                total = o_own[j]
                for copy in o_first if j == 0 else []:
                    copy.wait_recv()
                for copy in o_copies[j]:
                    copy.wait_recv()
                for o in range(n_tp - 1):
                    total = total + o_recv[l - 1, o, j].astype(F32)
                total = total.reshape(batch, cut)
                x = rounded(xs[:, span] + total)
            xs[:, span] = x
            squares = squares + jnp.sum(x * x, axis=1, keepdims=True)
            scaled = (x * gain[l : l + 1, span]).astype(BF16)
            gates = gates + dot(scaled, wif[l, span])
            if j == 0:
                for c in range(4):
                    w_loads[l][c].wait()

            def project(c):
                product = dot(scaled, w[l, c, span])
                if j:
                    product = product + p_own[l, c].reshape(batch, width)
                return product

            if j + 1 < len(steps):
                for c in range(4):
                    p_own[l, c] = project(c).reshape(n_dp, seqs, width)
                continue
            ahead = project(0)
            g_send[l] = jnp.where(iota((batch, LANES), 1) < 2 * heads, gates, squares).reshape(
                n_dp, seqs, LANES
            )
            for c in range(4):
                product, ahead = ahead, project(c + 1) if c < 3 else None
                send_products(c, product)
                if c == 0:
                    g_copies = [
                        send(
                            g_send.at[l, peer],
                            g_recv.at[l, i],
                            g_ss.at[l, i],
                            g_rs.at[l, i],
                            "dp",
                            peer,
                        )
                        for i, peer in enumerate(peers)
                    ]
                p_copies.append(start_products(c) if c < 2 else start_pairs(c))

        far_copies = [pass_pairs(c) for c in (2, 3)]

        if l + 1 < layers:
            start_loads(l + 1, 0, 4)
            m_loads[l + 1].start()
            start_loads(l + 1, 4, 5)

        for c in g_copies:
            c.wait_recv()
        g_sum = g_send[l, d]
        for i in range(n_dp - 1):
            g_sum = g_sum + g_recv[l, i]
        inv_rms = lax.rsqrt(g_sum[:, 2 * heads : 2 * heads + 1] / depth + EPS)
        input_pre = inv_rms * g_sum[:, 0:heads]
        forget_pre = inv_rms * g_sum[:, heads : 2 * heads] + bias[l : l + 1, :]
        log_forget = jnp.minimum(forget_pre, 0.0) - jnp.log1p(jnp.exp(-jnp.abs(forget_pre)))
        old_max = maxs[l]
        new_max = jnp.maximum(log_forget + old_max, input_pre)
        max_out[l] = new_max
        keep = column(jnp.exp(log_forget + old_max - new_max))
        admit = column(jnp.exp(input_pre - new_max))
        floor = column(jnp.exp(-new_max))
        if hp != heads:
            floor = jnp.where((iota((rows, 1), 0) & (hp - 1)) < heads, floor, 1.0)

        def stored(c):
            for copy in p_copies[c]:
                copy.wait_recv()
            total = p_own[l, c, d] + p_near[l, c]
            for i in range(n_dp - 2):
                total = total + p_recv[l, c, i].astype(F32)
            return rounded(inv_rms * total)

        def stored_pair(c):
            total = p_both[c - 2]
            for j, copy in enumerate(far_copies[c - 2]):
                copy.wait_recv()
                total = total + p_far[l, c - 2, j].astype(F32)
            return rounded(inv_rms * total)

        query = stored(0)
        m_loads[l].wait()
        query_rows = to_rows(query)
        query_low = query_rows.astype(BF16)
        old_inner = jnp.sum(over_heads(query * norm[l]) * mask[...], axis=1, keepdims=True)
        step = 2 * pair

        acc = jnp.zeros((seqs, heads, pair), F32)
        for j in range(square // step):
            qx = dot(query_low, spread[:, j * step : (j + 1) * step])
            for i in range(2):
                at = slice(j * step + i * pair, j * step + (i + 1) * pair)
                acc = acc + three(qx[:, i * pair : (i + 1) * pair]) * m[l, :, :, at]
        if hp != heads:
            acc = jnp.concatenate([acc, jnp.zeros((seqs, hp - heads, pair), F32)], axis=1)
        acc = acc.reshape(rows, pair)
        acc = acc + pltpu.roll(acc, hd, 1)

        key = stored(1) * hd ** (-0.5)
        key_rows = to_rows(key)
        match = jnp.sum(query_rows * key_rows, axis=1, keepdims=True) * (hd / pair)
        inner = keep * old_inner + admit * match
        bound = jnp.maximum(jnp.abs(inner), floor)
        fresh = match * admit / bound
        past = keep * acc / bound
        top = rounded(past)
        halves = jnp.where(iota((rows, pair), 1) < hd, top, past - top).astype(BF16)
        past_wide = from_rows(dot(halves, unfold[...]) * mask[...])
        fresh_wide = from_rows(fresh * mask[...])
        value = stored_pair(2)
        readout = past_wide + fresh_wide * value
        mix_all[l, d] = (readout * jax.nn.sigmoid(stored_pair(3))).astype(BF16)
        mix_copies = [
            send(
                mix_all.at[l, d],
                mix_all.at[l, d],
                mix_ss.at[l, i],
                mix_rs.at[l, i],
                "dp",
                peer,
            )
            for i, peer in enumerate(peers)
        ]
        w_loads[l][4].wait()
        if l + 1 < layers:
            o_first = []
            for i, e in enumerate((d, near)):
                if i:
                    mix_copies[-1].wait_recv()
                partial_out = dot(mix_all[l, e], w[l, 4])
                for j, span in enumerate(spans):
                    o_own[j, e] = partial_out[:, span]
                    o_send[l, j, e] = partial_out[:, span].astype(BF16)
                for o, peer in enumerate(tp_peers):
                    o_first.append(
                        send(
                            o_send.at[l, :, e],
                            o_recv.at[l, o, :, e],
                            first_ss.at[l, i, o],
                            first_rs.at[l, i, o],
                            "tp",
                            peer,
                        )
                    )
        norm_out[l] = from_rows(keep * mask[...]) * norm[l] + from_rows(admit * mask[...]) * key
        keep3 = three(jnp.broadcast_to(keep, (rows, pair)))
        admitted3 = three(admit * to_rows(value))
        key_low = key_rows.astype(BF16)

        for j in range(square // step):
            kx = dot(key_low, spread[:, j * step : (j + 1) * step])
            for i in range(2):
                at = slice(j * step + i * pair, j * step + (i + 1) * pair)
                part = three(kx[:, i * pair : (i + 1) * pair])
                m[l, :, :, at] = keep3 * m[l, :, :, at] + part * admitted3

        for c in mix_copies[: n_dp - 2 if l + 1 < layers else n_dp - 1]:
            c.wait_recv()
        if l + 1 < layers:
            mixed = [
                mix_all[l, pl.ds(e, 2)].astype(F32).reshape(2 * seqs, width).astype(BF16)
                for e in pairs
            ]
            o_copies = []
            for j, span in enumerate(spans):
                o_copies.append([])
                for i, e in enumerate(pairs):
                    partial_out = dot(mixed[i], w[l, 4, :, span]).reshape(2, seqs, cut)
                    o_own[j, pl.ds(e, 2)] = partial_out
                    o_send[l, j, pl.ds(e, 2)] = partial_out.astype(BF16)
                    for o, peer in enumerate(tp_peers):
                        o_copies[j].append(
                            send(
                                o_send.at[l, j, pl.ds(e, 2)],
                                o_recv.at[l, o, j, pl.ds(e, 2)],
                                o_ss.at[l, j, i, o],
                                o_rs.at[l, j, i, o],
                                "tp",
                                peer,
                            )
                        )
        else:
            mixed_all = mix_all[l].astype(F32).reshape(batch, width).astype(BF16)
            partial_out = dot(mixed_all, w[l, 4]).reshape(n_tp, rows_x, d_local)
            r_own[...] = partial_out
            r_send[...] = partial_out.astype(BF16)
            for o, peer in enumerate(tp_order):
                send(r_send.at[peer], r_recv.at[t], r_ss.at[o], r_rs.at[t], "tp", peer)
            total = r_own[t]
            for peer in tp_peers:
                arrived(r_recv.at[peer], r_ss.at[0], r_rs.at[peer], "tp", peer)
            for peer in tp_peers:
                total = total + r_recv[peer].astype(F32)
            own_rows = pl.ds(pl.multiple_of(t * rows_x, rows_x), rows_x)
            tok_out[...] = (xs[own_rows, :] + total).astype(BF16)

    for c in sends:
        c.wait_send()


def store(*refs):
    n = len(refs) // 2
    copies = [pltpu.make_async_copy(refs[i], refs[n + i], refs[-1].at[i]) for i in range(n)]
    for c in copies:
        c.start()
    for c in copies:
        c.wait()


def solution(mesh):
    n_tp, n_dp = mesh.shape["tp"], mesh.shape["dp"]

    def per_device(
        tokens,
        norm_gain,
        query_weight,
        key_weight,
        value_weight,
        outgate_weight,
        input_gate_weight,
        forget_gate_weight,
        forget_bias,
        out_weight,
        memory_state,
        normalizer_state,
        maximum_state,
    ):
        rows_x, d_local = tokens.shape
        layers, _, width = query_weight.shape
        _, seqs, heads, square = memory_state.shape
        hd = width // heads
        hp = -(-heads // 8) * 8
        batch = n_tp * rows_x
        pieces = 4 if d_local % 512 == 0 else 1
        sem = pltpu.SemaphoreType.DMA
        vmem = pltpu.VMEM
        anywhere = pl.BlockSpec(memory_space=pl.ANY)
        in_vmem = pl.BlockSpec(memory_space=pltpu.VMEM)
        results = [
            (tokens.shape, BF16),
            (memory_state.shape, F32),
            (normalizer_state.shape, F32),
            (maximum_state.shape, F32),
        ]
        room = memory_state.size * 4 + normalizer_state.size * 4
        limit = (60 << 20) + (3 << 20) - max(room, 3 << 20) - (256 << 10)
        held = pl.pallas_call(
            functools.partial(kernel, n_tp, n_dp),
            out_shape=tuple(vmem(*r) for r in results),
            in_specs=[anywhere] * 13,
            out_specs=(in_vmem,) * 4,
            scratch_shapes=[
                vmem((n_tp, rows_x, d_local), BF16),
                vmem((batch, d_local), F32),
                vmem(norm_gain.shape, F32),
                vmem((layers, 5, d_local, width), BF16),
                vmem((layers, heads, d_local), BF16),
                vmem((layers, heads, d_local), BF16),
                vmem((layers, d_local, LANES), BF16),
                vmem(forget_bias.shape, F32),
                vmem(normalizer_state.shape, F32),
                vmem(maximum_state.shape, F32),
                vmem((2 * hd, square), BF16),
                vmem((width, 2 * hd), BF16),
                vmem((2 * hd, width), BF16),
                vmem((seqs * hp, width), F32),
                vmem((layers, 4, n_dp, seqs, width), F32),
                vmem((layers, 2, n_dp, seqs, width), BF16),
                vmem((layers, 2, seqs, width), F32),
                vmem((layers, 2, n_dp - 2, seqs, width), BF16),
                vmem((layers, 2, n_dp // 2, seqs, width), F32),
                vmem((2, seqs, width), F32),
                vmem((layers, 2, n_dp // 2 - 1, seqs, width), BF16),
                vmem((layers, 2, n_dp // 2 - 1, seqs, width), BF16),
                vmem((layers, n_dp, seqs, LANES), F32),
                vmem((layers, n_dp - 1, seqs, LANES), F32),
                vmem((layers, n_dp, seqs, width), BF16),
                vmem((pieces, n_dp, seqs, d_local // pieces), F32),
                vmem((layers - 1, pieces, n_dp, seqs, d_local // pieces), BF16),
                vmem((layers - 1, n_tp - 1, pieces, n_dp, seqs, d_local // pieces), BF16),
                vmem((n_tp, rows_x, d_local), F32),
                vmem((n_tp, rows_x, d_local), BF16),
                vmem((n_tp, rows_x, d_local), BF16),
                sem((7,)),
                sem((layers, 5)),
                sem((layers,)),
                sem((n_tp - 1,)),
                sem((n_tp,)),
                sem((layers, 2, n_dp - 1)),
                sem((layers, 2, n_dp - 1)),
                sem((layers, n_dp - 1)),
                sem((layers, n_dp - 1)),
                sem((layers, n_dp - 1)),
                sem((layers, n_dp - 1)),
                sem((layers - 1, pieces, n_dp // 2 - 1, n_tp - 1)),
                sem((layers - 1, pieces, n_dp // 2 - 1, n_tp - 1)),
                sem((layers - 1, 2, n_tp - 1)),
                sem((layers - 1, 2, n_tp - 1)),
                sem((n_tp - 1,)),
                sem((n_tp,)),
                sem((layers, 2, n_dp // 2)),
                sem((layers, 2, n_dp // 2)),
                sem((layers, 2, n_dp // 2 - 1)),
                sem((layers, 2, n_dp // 2 - 1)),
            ],
            compiler_params=pltpu.CompilerParams(
                collective_id=0, has_side_effects=True, vmem_limit_bytes=limit
            ),
        )(
            tokens,
            norm_gain,
            query_weight,
            key_weight,
            value_weight,
            outgate_weight,
            jnp.swapaxes(input_gate_weight, 1, 2),
            jnp.swapaxes(forget_gate_weight, 1, 2),
            forget_bias,
            out_weight,
            memory_state,
            normalizer_state,
            maximum_state,
        )
        return pl.pallas_call(
            store,
            out_shape=tuple(jax.ShapeDtypeStruct(*r) for r in results),
            in_specs=[in_vmem] * 4,
            out_specs=(anywhere,) * 4,
            scratch_shapes=[sem((4,))],
            compiler_params=pltpu.CompilerParams(vmem_limit_bytes=1024 * 1024),
        )(*held)

    in_specs = (
        P(("grp", "tp"), "dp"),
        P(None, "dp"),
        P(None, "dp", "tp"),
        P(None, "dp", "tp"),
        P(None, "dp", "tp"),
        P(None, "dp", "tp"),
        P(None, "dp", "tp"),
        P(None, "dp", "tp"),
        P(None, "tp"),
        P(None, "tp", "dp"),
        P(None, ("grp", "dp"), "tp", None),
        P(None, ("grp", "dp"), "tp"),
        P(None, ("grp", "dp"), "tp"),
    )
    out_specs = (
        P(("grp", "tp"), "dp"),
        P(None, ("grp", "dp"), "tp", None),
        P(None, ("grp", "dp"), "tp"),
        P(None, ("grp", "dp"), "tp"),
    )
    return jax.shard_map(
        per_device, mesh=mesh, in_specs=in_specs, out_specs=out_specs, check_vma=False
    )
```

```python
import functools

import jax
import jax.numpy as jnp
from jax import lax
from jax.experimental import pallas as pl
from jax.experimental.pallas import tpu as pltpu
from jax.sharding import PartitionSpec as P

EPS = 1e-06
F32 = jnp.float32
BF16 = jnp.bfloat16
MESH = pl.DeviceIdType.MESH
LANES = 128


def dot(a, b):
    return jnp.dot(a, b, preferred_element_type=F32)


def dot_t(a, b):
    return lax.dot_general(a, b, (((1,), (1,)), ((), ())), preferred_element_type=F32)


def iota(shape, dim):
    return lax.broadcasted_iota(jnp.int32, shape, dim)


def kernel(
    n_tp,
    n_dp,
    tokens,
    gain_in,
    wq,
    wk,
    wv,
    wg,
    wi_in,
    wf_in,
    bias_in,
    wo,
    mem_in,
    norm_in,
    max_in,
    tok_out,
    m,
    norm_out,
    max_out,
    x_all,
    xs,
    gain,
    w,
    wi,
    wf,
    wif,
    bias,
    norm,
    maxs,
    spread,
    fold,
    unfold,
    mask,
    p_own,
    p_send,
    p_near,
    p_recv,
    p_pair,
    p_both,
    p_sum,
    p_far,
    g_send,
    g_recv,
    mix_all,
    o_own,
    o_send,
    o_recv,
    r_own,
    r_send,
    r_recv,
    load_sem,
    w_sem,
    m_sem,
    x_ss,
    x_rs,
    p_ss,
    p_rs,
    g_ss,
    g_rs,
    mix_ss,
    mix_rs,
    o_ss,
    o_rs,
    first_ss,
    first_rs,
    r_ss,
    r_rs,
    pair_ss,
    pair_rs,
    far_ss,
    far_rs,
):
    t = lax.axis_index("tp")
    d = lax.axis_index("dp")
    layers = wq.shape[0]
    rows_x, d_local = tokens.shape
    width = wq.shape[2]
    seqs, heads, square = mem_in.shape[1:]
    hd = width // heads
    hd_bits = hd.bit_length() - 1
    hp = mask.shape[0] // seqs
    rows = seqs * hp
    batch = n_tp * rows_x
    depth = d_local * n_dp
    pair = fold.shape[1]
    pieces = o_own.shape[0]
    cut = d_local // pieces
    spans = [slice(j * cut, (j + 1) * cut) for j in range(pieces)]

    loads = [
        pltpu.make_async_copy(src, dst, load_sem.at[i])
        for i, (src, dst) in enumerate(
            [
                (tokens, x_all.at[t]),
                (gain_in, gain),
                (wi_in, wi),
                (wf_in, wf),
                (bias_in, bias),
                (max_in, maxs),
                (norm_in, norm),
            ]
        )
    ]
    for c in loads:
        c.start()
    order = (wq, wk, wv, wg, wo)
    w_loads = [
        [pltpu.make_async_copy(order[c].at[l], w.at[l, c], w_sem.at[l, c]) for c in range(5)]
        for l in range(layers)
    ]
    m_loads = [pltpu.make_async_copy(mem_in.at[l], m.at[l], m_sem.at[l]) for l in range(layers)]

    def start_loads(l, first, last):
        for c in range(first, last):
            w_loads[l][c].start()

    start_loads(0, 0, 4)
    m_loads[0].start()
    barrier = pltpu.get_barrier_semaphore()
    for o in range(1, n_tp):
        pl.semaphore_signal(
            barrier, inc=1, device_id={"tp": lax.rem(t + o, n_tp)}, device_id_type=MESH
        )
    for o in range(1, n_dp):
        pl.semaphore_signal(
            barrier, inc=1, device_id={"dp": lax.rem(d + o, n_dp)}, device_id_type=MESH
        )
    pl.semaphore_wait(barrier, n_tp + n_dp - 2)
    loads[0].wait()

    def sibling(e):
        return e + 1 - 2 * lax.rem(e, 2)

    far = []
    for j in range(n_dp // 2):
        e = lax.rem(d + 2 * j, n_dp)
        if j:
            far.append(e)
            far.append(sibling(e))
    near = sibling(d)
    peers = far + [near]
    pairs = [2 * lax.rem(d // 2 + j, n_dp // 2) for j in range(1, n_dp // 2)]
    theirs = [near] + [lax.rem(d + 2 * j, n_dp) for j in range(1, n_dp // 2)]
    mine = [d] + [sibling(e) for e in theirs[1:]]
    tp_peers = [lax.rem(t + o, n_tp) for o in range(1, n_tp)]
    tp_order = tp_peers
    if n_tp % 2 == 0:
        half = n_tp // 2
        upper = t // half
        tp_order = [(1 - upper) * (n_tp - 1) + (2 * upper - 1) * j for j in range(half)]
        tp_order += [upper * half + lax.rem(t + o, half) for o in range(1, half)]

    sends = []

    def send(src, dst, ss, rs, axis, peer):
        copy = pltpu.make_async_remote_copy(
            src_ref=src,
            dst_ref=dst,
            send_sem=ss,
            recv_sem=rs,
            device_id={axis: peer},
            device_id_type=MESH,
        )
        copy.start()
        sends.append(copy)
        return copy

    def arrived(dst, ss, rs, axis, peer):
        pltpu.make_async_remote_copy(
            src_ref=dst,
            dst_ref=dst,
            send_sem=ss,
            recv_sem=rs,
            device_id={axis: peer},
            device_id_type=MESH,
        ).wait_recv()

    for o, peer in enumerate(tp_order):
        send(x_all.at[t], x_all.at[t], x_ss.at[o], x_rs.at[t], "tp", peer)
    start_loads(0, 4, 5)
    for l in range(1, layers):
        start_loads(l, 0, 4)
        m_loads[l].start()
        start_loads(l, 4, 5)

    spread[...] = jnp.where(
        lax.shift_right_logical(iota(spread.shape, 1), hd_bits) == iota(spread.shape, 0), 1.0, 0.0
    ).astype(BF16)
    fold[...] = jnp.where(
        (iota(fold.shape, 0) & (hd - 1)) == (iota(fold.shape, 1) & (hd - 1)), 1.0, 0.0
    ).astype(BF16)
    unfold[...] = jnp.where(
        (iota(unfold.shape, 0) & (hd - 1)) == (iota(unfold.shape, 1) & (hd - 1)), 1.0, 0.0
    ).astype(BF16)
    mask[...] = jnp.where(
        (iota(mask.shape, 0) & (hp - 1)) == lax.shift_right_logical(iota(mask.shape, 1), hd_bits),
        1.0,
        0.0,
    )

    def over_heads(z):
        return jnp.broadcast_to(z[:, None, :], (seqs, hp, z.shape[1])).reshape(rows, z.shape[1])

    def column(z):
        own = (iota((rows, heads), 0) & (hp - 1)) == iota((rows, heads), 1)
        return jnp.sum(jnp.where(own, over_heads(z), 0.0), axis=1, keepdims=True)

    def to_rows(z):
        return dot((over_heads(z) * mask[...]).astype(BF16), fold[...])

    def from_rows(z):
        return jnp.sum(z.reshape(seqs, hp, width), axis=1)

    def three(z):
        return z.reshape(seqs, hp, z.shape[1])[:, 0:heads]

    def rounded(z):
        return z.astype(BF16).astype(F32)

    for c in loads[1:]:
        c.wait()
    for l in range(layers):
        gate_rows = jnp.concatenate(
            [
                wi[l].astype(F32),
                wf[l].astype(F32),
                jnp.zeros((LANES - 2 * heads, d_local), F32),
            ],
            axis=0,
        )
        wif[l] = gate_rows.T.astype(BF16)

    o_copies = []
    for l in range(layers):
        squares = jnp.zeros((batch, 1), F32)
        gates = jnp.zeros((batch, LANES), F32)
        p_copies = []

        def send_products(c, product):
            own = product.reshape(n_dp, seqs, width)
            p_own[l, c] = own
            if c < 2:
                p_send[l, c] = own.astype(BF16)

        def start_products(c):
            n = len(far)
            return [
                send(
                    p_send.at[l, c, peer],
                    p_recv.at[l, c, i],
                    p_ss.at[l, c, i],
                    p_rs.at[l, c, i],
                    "dp",
                    peer,
                )
                for i, peer in enumerate(far)
            ] + [
                send(
                    p_own.at[l, c, sibling(d)],
                    p_near.at[l, c],
                    p_ss.at[l, c, n],
                    p_rs.at[l, c, n],
                    "dp",
                    sibling(d),
                )
            ]

        def start_pairs(c):
            return [
                send(
                    p_own.at[l, c, e],
                    p_pair.at[l, c - 2, j],
                    pair_ss.at[l, c - 2, j],
                    pair_rs.at[l, c - 2, j],
                    "dp",
                    near,
                )
                for j, e in enumerate(theirs)
            ]

        def pass_pairs(c):
            for copy in p_copies[c]:
                copy.wait_recv()
            p_both[c - 2] = p_own[l, c, d] + p_pair[l, c - 2, 0]
            copies = []
            for j in range(1, n_dp // 2):
                p_sum[l, c - 2, j - 1] = (p_own[l, c, mine[j]] + p_pair[l, c - 2, j]).astype(BF16)
                copies.append(
                    send(
                        p_sum.at[l, c - 2, j - 1],
                        p_far.at[l, c - 2, j - 1],
                        far_ss.at[l, c - 2, j - 1],
                        far_rs.at[l, c - 2, j - 1],
                        "dp",
                        mine[j],
                    )
                )
            return copies

        steps = spans if l else [slice(0, d_local)]
        for j, span in enumerate(steps):
            if l == 0:
                for peer in tp_peers:
                    arrived(x_all.at[peer], x_ss.at[0], x_rs.at[peer], "tp", peer)
                x = x_all[...].astype(F32).reshape(batch, d_local)
            else:
                total = o_own[j]
                for copy in o_first if j == 0 else []:
                    copy.wait_recv()
                for copy in o_copies[j]:
                    copy.wait_recv()
                for o in range(n_tp - 1):
                    total = total + o_recv[l - 1, o, j].astype(F32)
                total = total.reshape(batch, cut)
                x = rounded(xs[:, span] + total)
            xs[:, span] = x
            squares = squares + jnp.sum(x * x, axis=1, keepdims=True)
            scaled = (x * gain[l : l + 1, span]).astype(BF16)
            gates = gates + dot(scaled, wif[l, span])
            if j == 0:
                for c in range(4):
                    w_loads[l][c].wait()

            def project(c):
                product = dot(scaled, w[l, c, span])
                if j:
                    product = product + p_own[l, c].reshape(batch, width)
                return product

            if j + 1 < len(steps):
                for c in range(4):
                    p_own[l, c] = project(c).reshape(n_dp, seqs, width)
                continue
            ahead = project(0)
            g_send[l] = jnp.where(iota((batch, LANES), 1) < 2 * heads, gates, squares).reshape(
                n_dp, seqs, LANES
            )
            for c in range(4):
                product, ahead = ahead, project(c + 1) if c < 3 else None
                send_products(c, product)
                if c == 0:
                    g_copies = [
                        send(
                            g_send.at[l, peer],
                            g_recv.at[l, i],
                            g_ss.at[l, i],
                            g_rs.at[l, i],
                            "dp",
                            peer,
                        )
                        for i, peer in enumerate(peers)
                    ]
                p_copies.append(start_products(c) if c < 2 else start_pairs(c))

        far_copies = [pass_pairs(c) for c in (2, 3)]

        for c in g_copies:
            c.wait_recv()
        g_sum = g_send[l, d]
        for i in range(n_dp - 1):
            g_sum = g_sum + g_recv[l, i]
        inv_rms = lax.rsqrt(g_sum[:, 2 * heads : 2 * heads + 1] / depth + EPS)
        input_pre = inv_rms * g_sum[:, 0:heads]
        forget_pre = inv_rms * g_sum[:, heads : 2 * heads] + bias[l : l + 1, :]
        log_forget = jnp.minimum(forget_pre, 0.0) - jnp.log1p(jnp.exp(-jnp.abs(forget_pre)))
        old_max = maxs[l]
        new_max = jnp.maximum(log_forget + old_max, input_pre)
        max_out[l] = new_max
        keep = column(jnp.exp(log_forget + old_max - new_max))
        admit = column(jnp.exp(input_pre - new_max))
        floor = column(jnp.exp(-new_max))
        if hp != heads:
            floor = jnp.where((iota((rows, 1), 0) & (hp - 1)) < heads, floor, 1.0)

        def stored(c):
            for copy in p_copies[c]:
                copy.wait_recv()
            total = p_own[l, c, d] + p_near[l, c]
            for i in range(n_dp - 2):
                total = total + p_recv[l, c, i].astype(F32)
            return rounded(inv_rms * total)

        def stored_pair(c):
            total = p_both[c - 2]
            for j, copy in enumerate(far_copies[c - 2]):
                copy.wait_recv()
                total = total + p_far[l, c - 2, j].astype(F32)
            return rounded(inv_rms * total)

        query = stored(0)
        m_loads[l].wait()
        query_rows = to_rows(query)
        query_low = query_rows.astype(BF16)
        old_inner = jnp.sum(over_heads(query * norm[l]) * mask[...], axis=1, keepdims=True)
        step = 2 * pair

        acc = jnp.zeros((seqs, heads, pair), F32)
        for j in range(square // step):
            qx = dot(query_low, spread[:, j * step : (j + 1) * step])
            for i in range(2):
                at = slice(j * step + i * pair, j * step + (i + 1) * pair)
                acc = acc + three(qx[:, i * pair : (i + 1) * pair]) * m[l, :, :, at]
        if hp != heads:
            acc = jnp.concatenate([acc, jnp.zeros((seqs, hp - heads, pair), F32)], axis=1)
        acc = acc.reshape(rows, pair)
        acc = acc + pltpu.roll(acc, hd, 1)

        key = stored(1) * hd ** (-0.5)
        key_rows = to_rows(key)
        match = jnp.sum(query_rows * key_rows, axis=1, keepdims=True) * (hd / pair)
        inner = keep * old_inner + admit * match
        bound = jnp.maximum(jnp.abs(inner), floor)
        fresh = match * admit / bound
        past = keep * acc / bound
        top = rounded(past)
        halves = jnp.where(iota((rows, pair), 1) < hd, top, past - top).astype(BF16)
        past_wide = from_rows(dot(halves, unfold[...]) * mask[...])
        fresh_wide = from_rows(fresh * mask[...])
        value = stored_pair(2)
        readout = past_wide + fresh_wide * value
        mix_all[l, d] = (readout * jax.nn.sigmoid(stored_pair(3))).astype(BF16)
        mix_copies = [
            send(
                mix_all.at[l, d],
                mix_all.at[l, d],
                mix_ss.at[l, i],
                mix_rs.at[l, i],
                "dp",
                peer,
            )
            for i, peer in enumerate(peers)
        ]
        w_loads[l][4].wait()
        if l + 1 < layers:
            o_first = []
            for i, e in enumerate((d, near)):
                if i:
                    mix_copies[-1].wait_recv()
                partial_out = dot(mix_all[l, e], w[l, 4])
                for j, span in enumerate(spans):
                    o_own[j, e] = partial_out[:, span]
                    o_send[l, j, e] = partial_out[:, span].astype(BF16)
                for o in (1, 0, 2):
                    peer = tp_peers[o]
                    o_first.append(
                        send(
                            o_send.at[l, :, e],
                            o_recv.at[l, o, :, e],
                            first_ss.at[l, i, o],
                            first_rs.at[l, i, o],
                            "tp",
                            peer,
                        )
                    )
        norm_out[l] = from_rows(keep * mask[...]) * norm[l] + from_rows(admit * mask[...]) * key
        keep3 = three(jnp.broadcast_to(keep, (rows, pair)))
        admitted3 = three(admit * to_rows(value))
        key_low = key_rows.astype(BF16)

        for j in range(square // step):
            kx = dot(key_low, spread[:, j * step : (j + 1) * step])
            for i in range(2):
                at = slice(j * step + i * pair, j * step + (i + 1) * pair)
                part = three(kx[:, i * pair : (i + 1) * pair])
                m[l, :, :, at] = keep3 * m[l, :, :, at] + part * admitted3

        for c in mix_copies[: n_dp - 2 if l + 1 < layers else n_dp - 1]:
            c.wait_recv()
        if l + 1 < layers:
            mixed = [
                mix_all[l, pl.ds(e, 2)].astype(F32).reshape(2 * seqs, width).astype(BF16)
                for e in pairs
            ]
            o_copies = []
            for j, span in enumerate(spans):
                o_copies.append([])
                for i, e in enumerate(pairs):
                    partial_out = dot(mixed[i], w[l, 4, :, span]).reshape(2, seqs, cut)
                    o_own[j, pl.ds(e, 2)] = partial_out
                    o_send[l, j, pl.ds(e, 2)] = partial_out.astype(BF16)
                    for o in (1, 0, 2):
                        peer = tp_peers[o]
                        o_copies[j].append(
                            send(
                                o_send.at[l, j, pl.ds(e, 2)],
                                o_recv.at[l, o, j, pl.ds(e, 2)],
                                o_ss.at[l, j, i, o],
                                o_rs.at[l, j, i, o],
                                "tp",
                                peer,
                            )
                        )
        else:
            mixed_all = mix_all[l].astype(F32).reshape(batch, width).astype(BF16)
            partial_out = dot(mixed_all, w[l, 4]).reshape(n_tp, rows_x, d_local)
            r_own[...] = partial_out
            r_send[...] = partial_out.astype(BF16)
            for o, peer in enumerate(tp_order):
                send(r_send.at[peer], r_recv.at[t], r_ss.at[o], r_rs.at[t], "tp", peer)
            for c in sends[: 1 - n_tp]:
                c.wait_send()
            total = r_own[t]
            for peer in tp_peers:
                arrived(r_recv.at[peer], r_ss.at[0], r_rs.at[peer], "tp", peer)
            for peer in tp_peers:
                total = total + r_recv[peer].astype(F32)
            own_rows = pl.ds(pl.multiple_of(t * rows_x, rows_x), rows_x)
            tok_out[...] = (xs[own_rows, :] + total).astype(BF16)

    for c in sends[1 - n_tp :]:
        c.wait_send()


def store(*refs):
    n = len(refs) // 2
    copies = [pltpu.make_async_copy(refs[i], refs[n + i], refs[-1].at[i]) for i in range(n)]
    for c in copies:
        c.start()
    for c in copies:
        c.wait()


def solution(mesh):
    n_tp, n_dp = mesh.shape["tp"], mesh.shape["dp"]

    def per_device(
        tokens,
        norm_gain,
        query_weight,
        key_weight,
        value_weight,
        outgate_weight,
        input_gate_weight,
        forget_gate_weight,
        forget_bias,
        out_weight,
        memory_state,
        normalizer_state,
        maximum_state,
    ):
        rows_x, d_local = tokens.shape
        layers, _, width = query_weight.shape
        _, seqs, heads, square = memory_state.shape
        hd = width // heads
        hp = -(-heads // 8) * 8
        batch = n_tp * rows_x
        pieces = 4 if d_local % 512 == 0 else 1
        sem = pltpu.SemaphoreType.DMA
        vmem = pltpu.VMEM
        anywhere = pl.BlockSpec(memory_space=pl.ANY)
        in_vmem = pl.BlockSpec(memory_space=pltpu.VMEM)
        results = [
            (tokens.shape, BF16),
            (memory_state.shape, F32),
            (normalizer_state.shape, F32),
            (maximum_state.shape, F32),
        ]
        room = memory_state.size * 4 + normalizer_state.size * 4
        limit = (60 << 20) + (3 << 20) - max(room, 3 << 20) - (256 << 10)
        held = pl.pallas_call(
            functools.partial(kernel, n_tp, n_dp),
            out_shape=tuple(vmem(*r) for r in results),
            in_specs=[anywhere] * 13,
            out_specs=(in_vmem,) * 4,
            scratch_shapes=[
                vmem((n_tp, rows_x, d_local), BF16),
                vmem((batch, d_local), F32),
                vmem(norm_gain.shape, F32),
                vmem((layers, 5, d_local, width), BF16),
                vmem((layers, heads, d_local), BF16),
                vmem((layers, heads, d_local), BF16),
                vmem((layers, d_local, LANES), BF16),
                vmem(forget_bias.shape, F32),
                vmem(normalizer_state.shape, F32),
                vmem(maximum_state.shape, F32),
                vmem((2 * hd, square), BF16),
                vmem((width, 2 * hd), BF16),
                vmem((2 * hd, width), BF16),
                vmem((seqs * hp, width), F32),
                vmem((layers, 4, n_dp, seqs, width), F32),
                vmem((layers, 2, n_dp, seqs, width), BF16),
                vmem((layers, 2, seqs, width), F32),
                vmem((layers, 2, n_dp - 2, seqs, width), BF16),
                vmem((layers, 2, n_dp // 2, seqs, width), F32),
                vmem((2, seqs, width), F32),
                vmem((layers, 2, n_dp // 2 - 1, seqs, width), BF16),
                vmem((layers, 2, n_dp // 2 - 1, seqs, width), BF16),
                vmem((layers, n_dp, seqs, LANES), F32),
                vmem((layers, n_dp - 1, seqs, LANES), F32),
                vmem((layers, n_dp, seqs, width), BF16),
                vmem((pieces, n_dp, seqs, d_local // pieces), F32),
                vmem((layers - 1, pieces, n_dp, seqs, d_local // pieces), BF16),
                vmem((layers - 1, n_tp - 1, pieces, n_dp, seqs, d_local // pieces), BF16),
                vmem((n_tp, rows_x, d_local), F32),
                vmem((n_tp, rows_x, d_local), BF16),
                vmem((n_tp, rows_x, d_local), BF16),
                sem((7,)),
                sem((layers, 5)),
                sem((layers,)),
                sem((n_tp - 1,)),
                sem((n_tp,)),
                sem((layers, 2, n_dp - 1)),
                sem((layers, 2, n_dp - 1)),
                sem((layers, n_dp - 1)),
                sem((layers, n_dp - 1)),
                sem((layers, n_dp - 1)),
                sem((layers, n_dp - 1)),
                sem((layers - 1, pieces, n_dp // 2 - 1, n_tp - 1)),
                sem((layers - 1, pieces, n_dp // 2 - 1, n_tp - 1)),
                sem((layers - 1, 2, n_tp - 1)),
                sem((layers - 1, 2, n_tp - 1)),
                sem((n_tp - 1,)),
                sem((n_tp,)),
                sem((layers, 2, n_dp // 2)),
                sem((layers, 2, n_dp // 2)),
                sem((layers, 2, n_dp // 2 - 1)),
                sem((layers, 2, n_dp // 2 - 1)),
            ],
            compiler_params=pltpu.CompilerParams(
                collective_id=0, has_side_effects=True, vmem_limit_bytes=limit
            ),
        )(
            tokens,
            norm_gain,
            query_weight,
            key_weight,
            value_weight,
            outgate_weight,
            jnp.swapaxes(input_gate_weight, 1, 2),
            jnp.swapaxes(forget_gate_weight, 1, 2),
            forget_bias,
            out_weight,
            memory_state,
            normalizer_state,
            maximum_state,
        )
        return pl.pallas_call(
            store,
            out_shape=tuple(jax.ShapeDtypeStruct(*r) for r in results),
            in_specs=[in_vmem] * 4,
            out_specs=(anywhere,) * 4,
            scratch_shapes=[sem((4,))],
            compiler_params=pltpu.CompilerParams(vmem_limit_bytes=1024 * 1024),
        )(*held)

    in_specs = (
        P(("grp", "tp"), "dp"),
        P(None, "dp"),
        P(None, "dp", "tp"),
        P(None, "dp", "tp"),
        P(None, "dp", "tp"),
        P(None, "dp", "tp"),
        P(None, "dp", "tp"),
        P(None, "dp", "tp"),
        P(None, "tp"),
        P(None, "tp", "dp"),
        P(None, ("grp", "dp"), "tp", None),
        P(None, ("grp", "dp"), "tp"),
        P(None, ("grp", "dp"), "tp"),
    )
    out_specs = (
        P(("grp", "tp"), "dp"),
        P(None, ("grp", "dp"), "tp", None),
        P(None, ("grp", "dp"), "tp"),
        P(None, ("grp", "dp"), "tp"),
    )
    return jax.shard_map(
        per_device, mesh=mesh, in_specs=in_specs, out_specs=out_specs, check_vma=False
    )
```
